32 devices in a mesh: sp: 16 (over z, y, core), tp: 2 (over x).
Axes of the slice: x: 2, y: 2, z: 4, core: 2. Of those that a mesh axis runs over, the one named last changes fastest.
Arguments:
- glu_value: bfloat16 [8192, 1024], P('sp', 'tp'), may hold values from -6 to 6
- glu_gate: bfloat16 [8192, 1024], P('sp', 'tp'), may hold values from -8 to 8
- conv_taps: float32 [31, 1024], P(None, 'tp'), may hold values from -1 to 1
- channel_norm_gain: float32 [1024], P('tp'), may hold values from 0.1 to 1.9
- channel_norm_bias: float32 [1024], P('tp'), may hold values from -3 to 3
- out_proj: bfloat16 [1024, 2048], P('tp'), may hold values from -0.1875 to 0.1875
- out_grad: bfloat16 [8192, 2048], P('sp'), may hold values from -6 to 6
Outputs:
- grad_value: bfloat16 [8192, 1024], P('sp', 'tp')
- grad_gate: bfloat16 [8192, 1024], P('sp', 'tp')
- grad_taps: float32 [31, 1024], P(None, 'tp')
- norm_gain_gradient: float32 [1024], P('tp')
- grad_bias: float32 [1024], P('tp')
- grad_proj: float32 [2048, 1024], P('sp', 'tp')
The draws below stay inside these ranges and needn't reach their ends.
All inputs are finite; a program needn't handle non-finite values.
Results may differ from the reference program's by a relative error of at most 0.0049.
Values may be sent and summed in bfloat16 or wider, within the bound.
A program may use at most 64 MiB of HBM per device.

```python
import jax
import jax.numpy as jnp
from jax import lax

D = 2048
CONV_CHANNELS = 1024
TAPS = 31
TOK_DEV = 512
SEQ = 8192


def spiked(result, rng, source, target, blocks, factor):
    def block_of(position):
        return (jnp.arange(result.shape[position]) // (result.shape[position] // blocks)).reshape((-1,) + (1,) * (result.ndim - 1 - position))

    one_side = jax.random.permutation(rng, blocks)[block_of(target)]
    far = (block_of(target) + blocks // 2) % blocks
    return jnp.where((block_of(source) == one_side) | (block_of(source) == far), factor * result, result)


def block_scale(own_key, dims, split, least, top_value):
    level, own = 1.0, jax.random.fold_in(own_key, 6)
    for dim, blocks in split:
        draws = jnp.exp(jax.random.uniform(jax.random.fold_in(own, dim), (blocks,), jnp.float32, least / len(split), top_value / len(split)))
        level = level * jnp.repeat(draws, dims[dim] // blocks).reshape([-1 if axis == dim else 1 for axis in range(len(dims))])
    return level


def gaussian(own_key, extent, deviation, limit, split=(), kind=jnp.bfloat16):
    values = deviation * jax.random.normal(own_key, extent, jnp.float32)
    if split:
        values = values * block_scale(own_key, extent, split, -0.22, 0.18)
    return jnp.clip(values, -limit, limit).astype(kind)


def gaussian_with(stream_key, extent, scale, most, pieces, heavy, held_as=jnp.bfloat16):
    result = scale * jax.random.normal(stream_key, extent, jnp.float32)
    if pieces:
        result = result * block_scale(stream_key, extent, pieces, -0.22, 0.18)
    return jnp.clip(spiked(result, jax.random.fold_in(stream_key, 3), *heavy), -most, most).astype(held_as)


def setup_inputs(seed: int = 0) -> dict:
    arg_keys = jax.random.split(jax.random.key(seed), 8)
    glu_value = gaussian(arg_keys[0], (SEQ, CONV_CHANNELS), 1.0, 6.0, ((0, 16), (1, 2)))
    glu_gate = gaussian(arg_keys[1], (SEQ, CONV_CHANNELS), 1.5, 8.0, ((0, 16), (1, 2)))
    conv_taps = gaussian(arg_keys[2], (TAPS, CONV_CHANNELS), TAPS ** -0.5, 1.0, ((1, 2),), jnp.float32)
    channel_norm_gain = jnp.clip(1.0 + 0.18 * jax.random.normal(arg_keys[3], (CONV_CHANNELS,), jnp.float32), 0.1, 1.9)
    channel_norm_bias = gaussian(arg_keys[4], (CONV_CHANNELS,), 0.5, 3.0, ((0, 2),), jnp.float32)
    out_proj = gaussian(arg_keys[5], (CONV_CHANNELS, D), CONV_CHANNELS ** -0.5, 0.1875, ((0, 2),))
    out_grad = gaussian_with(arg_keys[6], (SEQ, D), 1.0, 6.0, ((0, 16),), (0, 1, 16, 2.0))
    return dict(glu_value=glu_value, glu_gate=glu_gate, conv_taps=conv_taps, channel_norm_gain=channel_norm_gain, channel_norm_bias=channel_norm_bias, out_proj=out_proj, out_grad=out_grad)


def rows_at(array, first, count, length):
    index = first + jnp.arange(count, dtype=jnp.int32)
    valid = jnp.logical_and(index >= 0, index < length)
    taken = jnp.take(array, jnp.clip(index, 0, length - 1), axis=0)
    return jnp.where(valid[:, None], taken, jnp.zeros_like(taken))

def reference(glu_value, glu_gate, conv_taps, channel_norm_gain, channel_norm_bias, out_proj, out_grad):
    length = glu_value.shape[0]
    blocks = length // TOK_DEV
    span = TOK_DEV + TAPS - 1
    window = span + TAPS - 1

    def step(carry, block):
        proj_acc, taps_acc, gain_acc, bias_acc = carry
        first = (block * TOK_DEV).astype(jnp.int32)
        value = rows_at(glu_value, first - (TAPS - 1), window, length).astype(jnp.float32)
        sig_gate = jax.nn.sigmoid(rows_at(glu_gate, first - (TAPS - 1), window, length).astype(jnp.float32))
        gated = (value * sig_gate).astype(jnp.bfloat16).astype(jnp.float32)
        conv_output = jnp.zeros((span, CONV_CHANNELS), jnp.float32)
        for k in range(TAPS):
            conv_output = conv_output + conv_taps[k][None, :] * gated[k:k + span]
        channel_mean = lax.optimization_barrier(jnp.mean(conv_output, axis=1, keepdims=True))
        var = lax.optimization_barrier(jnp.mean(conv_output * conv_output, axis=1, keepdims=True)) - channel_mean * channel_mean
        inverse_deviation = lax.rsqrt(var + 1e-05)
        centered = (conv_output - channel_mean) * inverse_deviation
        normalized_rows = centered * channel_norm_gain[None, :] + channel_norm_bias[None, :]
        sig_norm = jax.nn.sigmoid(normalized_rows)
        act = (normalized_rows * sig_norm).astype(jnp.bfloat16)
        grad_rows = rows_at(out_grad, first, span, length)
        grad_act = jnp.dot(grad_rows, out_proj.T, preferred_element_type=jnp.float32)
        normalized_gradient = grad_act * sig_norm * (1.0 + normalized_rows * (1.0 - sig_norm))
        scaled_rows = normalized_gradient * channel_norm_gain[None, :]
        conv_gradient = inverse_deviation * (scaled_rows - lax.optimization_barrier(jnp.mean(scaled_rows, axis=1, keepdims=True)) - centered * lax.optimization_barrier(jnp.mean(scaled_rows * centered, axis=1, keepdims=True)))
        own_grad = conv_gradient[:TOK_DEV]
        proj_acc = proj_acc + jnp.dot(grad_rows[:TOK_DEV].T, act[:TOK_DEV], preferred_element_type=jnp.float32)
        gain_acc = gain_acc + lax.optimization_barrier(jnp.sum(normalized_gradient[:TOK_DEV] * centered[:TOK_DEV], axis=0))
        bias_acc = bias_acc + lax.optimization_barrier(jnp.sum(normalized_gradient[:TOK_DEV], axis=0))
        taps_acc = taps_acc + jnp.stack([lax.optimization_barrier(jnp.sum(own_grad * gated[k:k + TOK_DEV], axis=0)) for k in range(TAPS)], axis=0)
        grad_gated = jnp.zeros((TOK_DEV, CONV_CHANNELS), jnp.float32)
        for k in range(TAPS):
            grad_gated = grad_gated + conv_taps[k][None, :] * conv_gradient[TAPS - 1 - k:TAPS - 1 - k + TOK_DEV]
        own_value = value[TAPS - 1:TAPS - 1 + TOK_DEV]
        own_sig = sig_gate[TAPS - 1:TAPS - 1 + TOK_DEV]
        grad_value = (grad_gated * own_sig).astype(jnp.bfloat16)
        grad_gate = (grad_gated * own_value * own_sig * (1.0 - own_sig)).astype(jnp.bfloat16)
        return ((proj_acc, taps_acc, gain_acc, bias_acc), (grad_value, grad_gate))
    init = (jnp.zeros((D, CONV_CHANNELS), jnp.float32), jnp.zeros((TAPS, CONV_CHANNELS), jnp.float32), jnp.zeros((CONV_CHANNELS,), jnp.float32), jnp.zeros((CONV_CHANNELS,), jnp.float32))
    (grad_proj, grad_taps, norm_gain_gradient, grad_bias), (value_blocks, gate_blocks) = lax.scan(step, init, jnp.arange(blocks, dtype=jnp.int32))
    grad_value = value_blocks.reshape(length, CONV_CHANNELS)
    grad_gate = gate_blocks.reshape(length, CONV_CHANNELS)
    return (grad_value, grad_gate, grad_taps, norm_gain_gradient, grad_bias, grad_proj)
```

```python
import functools

import jax
import jax.numpy as jnp
from jax import lax
from jax.experimental import pallas as pl
from jax.experimental.pallas import tpu as pltpu
from jax.sharding import PartitionSpec as P

LANES = 128
HALO = 32
SMALL = 40
MESH = pl.DeviceIdType.MESH
F32, BF16 = jnp.float32, jnp.bfloat16


def kernel(
    n, tp, taps_n,
    value_hbm, gate_hbm, taps_ref, gain_ref, bias_ref, proj_hbm, grad_hbm,
    gv_hbm, gg_hbm, small_hbm, gp_hbm,
    value, gate, proj, grad, gpad, conv, gact, gnorm, gcpad, act,
    full, pair_out, pair_in, ring_out, ring_in,
    halo_out, halo_in, back_out, back_in,
    stage, mean_b, rstd_b, stat_out, stat_in, stat2_out, stat2_in,
    tacc, small, small_in, small_all, small_fin, small_tot,
    gv, gg, gp,
    in_sem, out_sem, halo_sem, back_sem, stat_sem, stat2_sem,
    pair_s, pair_r, ring_s, ring_r, sp_sem, sa_s, sa_r, sf_sem,
):
    rows, width = value.shape
    blocks = width // LANES
    chunks = rows // LANES
    nc = n // 2
    half = blocks // 2
    share = full.shape[1]
    model = grad.shape[1]
    channels = width * tp
    me = lax.axis_index("sp")
    col = lax.axis_index("tp")
    par = lax.rem(me, 2)
    chip = me // 2
    partner = chip * 2 + 1 - par
    nxt = lax.rem(me + 1, n)
    prv = lax.rem(me + n - 1, n)

    loads = [
        pltpu.make_async_copy(s, d, in_sem.at[i])
        for i, (s, d) in enumerate(
            ((value_hbm, value), (gate_hbm, gate), (grad_hbm, grad), (proj_hbm, proj))
        )
    ]
    for c in loads:
        c.start()

    barrier = pltpu.get_barrier_semaphore()

    @pl.loop(1, n)
    def _(i):
        pl.semaphore_signal(
            barrier, inc=1, device_id={"sp": lax.rem(me + i, n)}, device_id_type=MESH
        )

    for t in range(1, tp):
        pl.semaphore_signal(
            barrier, inc=1, device_id={"tp": lax.rem(col + t, tp)}, device_id_type=MESH
        )

    def remote(src, dst, s, r, where):
        return pltpu.make_async_remote_copy(
            src_ref=src, dst_ref=dst, send_sem=s, recv_sem=r,
            device_id=where, device_id_type=MESH,
        )

    def lanes(cb):
        return pl.ds(pl.multiple_of(cb * LANES, LANES), LANES)

    def stat_copy(out, inn, sem, j, t):
        return remote(
            out.at[j], inn.at[j, t - 1], sem.at[0, j, t - 1], sem.at[1, j, t - 1],
            {"tp": lax.rem(col + t, tp)},
        )

    sub = lax.broadcasted_iota(jnp.int32, (8, LANES), 0)

    def send_stats(out, inn, sem, j):
        a = jnp.sum(stage[0].T, axis=0, keepdims=True)
        b = jnp.sum(stage[1].T, axis=0, keepdims=True)
        out[j] = jnp.where(sub == 0, a, b)
        for t in range(1, tp):
            stat_copy(out, inn, sem, j, t).start()

    def recv_stats(out, inn, sem, j):
        total = out[j]
        for t in range(1, tp):
            stat_copy(out, inn, sem, j, t).wait()
            total = total + inn[j, t - 1]
        total = total / channels
        return total[0:1], total[1:2]

    loads[0].wait()
    loads[1].wait()

    def gated_rows(r0, cb, count):
        v = value[pl.ds(r0, count), lanes(cb)].astype(F32)
        s = jax.nn.sigmoid(gate[pl.ds(r0, count), lanes(cb)].astype(F32))
        return (v * s).astype(BF16)

    for cb in range(blocks):
        g = gated_rows(rows - HALO, cb, HALO)
        halo_out[cb] = g
    pl.semaphore_wait(barrier, n - 1 + tp - 1)
    halo = remote(halo_out, halo_in, halo_sem.at[0], halo_sem.at[1], {"sp": nxt})
    halo.start()

    @pl.loop(0, rows // 64)
    def _(i):
        r0 = pl.multiple_of(i * 64, 64)
        for cb in range(blocks):
            gpad[cb, pl.ds(r0 + HALO, 64), :] = gated_rows(r0, cb, 64).astype(F32)

    def tap_row(k, cb):
        return taps_ref[pl.ds(k, 1), lanes(cb)]

    def conv_chunk(j):
        for h in range(LANES // 64):
            r0 = j * LANES + h * 64

            def body(cb, carry):
                s, q = carry
                acc = tap_row(0, cb) * gpad[cb, pl.ds(r0 + 2, 64), :]
                for k in range(1, taps_n):
                    acc = acc + tap_row(k, cb) * gpad[cb, pl.ds(r0 + HALO - taps_n + 1 + k, 64), :]
                conv[cb, pl.ds(r0, 64), :] = acc
                return s + acc, q + acc * acc

            zero = jnp.zeros((64, LANES), F32)
            s, q = lax.fori_loop(0, blocks, body, (zero, zero))
            stage[0, pl.ds(h * 64, 64), :] = s
            stage[1, pl.ds(h * 64, 64), :] = q
        send_stats(stat_out, stat_in, stat_sem, j)

    order = list(range(1, chunks)) + [0]
    for j in order:
        if j == 0:
            halo.wait()
            first = me == 0
            for cb in range(blocks):
                h = halo_in[cb].astype(F32)
                gpad[cb, pl.ds(0, HALO), :] = jnp.where(first, jnp.zeros_like(h), h)
        conv_chunk(j)

    loads[2].wait()
    loads[3].wait()
    for cb in range(blocks):
        gact[cb] = lax.dot_general(
            grad[...], proj[pl.ds(cb * LANES, LANES), :], (((1,), (1,)), ((), ())),
            preferred_element_type=F32,
        )

    tacc[...] = jnp.zeros_like(tacc)

    def norm_chunk(j):
        mean, sq = recv_stats(stat_out, stat_in, stat_sem, j)
        rstd = lax.rsqrt(sq - mean * mean + 1e-05)
        mean_b[...] = jnp.broadcast_to(mean, (LANES, LANES)).T
        rstd_b[pl.ds(j * LANES, LANES), :] = jnp.broadcast_to(rstd, (LANES, LANES)).T

        @pl.loop(0, LANES // 32)
        def _(h):
            l0 = pl.multiple_of(h * 32, 32)
            r0 = pl.multiple_of(j * LANES + l0, 32)
            m = mean_b[pl.ds(l0, 32), :]
            rs = rstd_b[pl.ds(r0, 32), :]
            s1 = jnp.zeros((32, LANES), F32)
            s2 = jnp.zeros((32, LANES), F32)
            for cb in range(blocks):
                cols = pl.ds(cb * LANES, LANES)
                gain = gain_ref[:, cols]
                xhat = (conv[cb, pl.ds(r0, 32), :] - m) * rs
                nrm = xhat * gain + bias_ref[:, cols]
                sig = jax.nn.sigmoid(nrm)
                act[pl.ds(r0, 32), cols] = (nrm * sig).astype(BF16)
                gn = gact[cb, pl.ds(r0, 32), :] * sig * (1.0 + nrm * (1.0 - sig))
                conv[cb, pl.ds(r0, 32), :] = xhat
                gx = gn * gain
                gnorm[cb, pl.ds(r0, 32), :] = gx
                gxx = gx * xhat
                s1 = s1 + gx
                s2 = s2 + gxx
                tacc[cb, taps_n] += jnp.sum((gn * xhat).reshape(4, 8, LANES), axis=0)
                tacc[cb, taps_n + 1] += jnp.sum(gn.reshape(4, 8, LANES), axis=0)
            stage[0, pl.ds(l0, 32), :] = s1
            stage[1, pl.ds(l0, 32), :] = s2

        send_stats(stat2_out, stat2_in, stat2_sem, j)

    for j in order:
        norm_chunk(j)

    per = LANES // share

    @pl.loop(0, model // LANES)
    def _(b):
        part = lax.dot_general(
            grad[:, lanes(b)], act[...], (((0,), (0,)), ((), ())),
            preferred_element_type=F32,
        )
        full[pl.ds(b * per, per)] = part.reshape(per, share, width)

    def pair_copy(i):
        return remote(
            pair_out.at[i], pair_in.at[i], pair_s.at[i], pair_r.at[i], {"sp": partner}
        )

    def ring_copy(i):
        return remote(
            ring_out.at[i], ring_in.at[i], ring_s.at[i], ring_r.at[i],
            {"sp": lax.rem(chip + i, nc) * 2 + par},
        )

    @pl.loop(0, nc)
    def _(i):
        dest = lax.rem(chip + i, nc)
        pair_out[i] = full[dest * 2 + 1 - par].astype(BF16)
        pair_copy(i).start()

    def gconv_chunk(j):
        m1, m2 = recv_stats(stat2_out, stat2_in, stat2_sem, j)
        stage[0] = jnp.broadcast_to(m1, (LANES, LANES)).T
        stage[1] = jnp.broadcast_to(m2, (LANES, LANES)).T

        @pl.loop(0, LANES // 64)
        def _(h):
            l0 = pl.multiple_of(h * 64, 64)
            r0 = pl.multiple_of(j * LANES + l0, 64)
            a = stage[0, pl.ds(l0, 64), :]
            b = stage[1, pl.ds(l0, 64), :]
            rs = rstd_b[pl.ds(r0, 64), :]
            for cb in range(blocks):
                gcpad[cb, pl.ds(r0, 64), :] = rs * (
                    gnorm[cb, pl.ds(r0, 64), :] - a - conv[cb, pl.ds(r0, 64), :] * b
                )

    gconv_chunk(0)
    for cb in range(blocks):
        back_out[cb] = gcpad[cb, pl.ds(0, HALO), :]
    back = remote(back_out, back_in, back_sem.at[0], back_sem.at[1], {"sp": prv})
    back.start()

    @pl.loop(1, nc)
    def _(i):
        dest = lax.rem(chip + i, nc)
        pair_copy(i).wait()
        ring_out[i] = (full[dest * 2 + par] + pair_in[i].astype(F32)).astype(BF16)
        ring_copy(i).start()

    for j in range(1, chunks):
        gconv_chunk(j)

    @pl.loop(0, rows // 64)
    def _(i):
        r0 = pl.multiple_of(i * 64, 64)

        @pl.loop(0, blocks)
        def _(cb):
            gc = gcpad[cb, pl.ds(r0, 64), :]
            for k in range(taps_n):
                prod = gc * gpad[cb, pl.ds(r0 + HALO - taps_n + 1 + k, 64), :]
                tacc[cb, k] += jnp.sum(prod.reshape(8, 8, LANES), axis=0)

    small[...] = jnp.zeros_like(small)
    for cb in range(blocks):
        small[cb, pl.ds(0, taps_n + 2), :] = jnp.sum(tacc[cb], axis=1)
    to_pair = remote(
        small.at[pl.ds((1 - par) * half, half)], small_in, sp_sem.at[0], sp_sem.at[1],
        {"sp": partner},
    )
    to_pair.start()

    def gated_gradient(j):
        @pl.loop(0, LANES // 64)
        def _(h):
            r0 = pl.multiple_of(j * LANES + h * 64, 64)

            @pl.loop(0, blocks)
            def _(cb):
                acc = tap_row(0, cb) * gcpad[cb, pl.ds(r0 + taps_n - 1, 64), :]
                for k in range(1, taps_n):
                    acc = acc + tap_row(k, cb) * gcpad[cb, pl.ds(r0 + taps_n - 1 - k, 64), :]
                v = value[pl.ds(r0, 64), lanes(cb)].astype(F32)
                s = jax.nn.sigmoid(gate[pl.ds(r0, 64), lanes(cb)].astype(F32))
                ds = acc * s
                gv[pl.ds(r0, 64), lanes(cb)] = ds.astype(BF16)
                gg[pl.ds(r0, 64), lanes(cb)] = (ds * v * (1.0 - s)).astype(BF16)

        span = pl.ds(j * LANES, LANES)
        return [
            pltpu.make_async_copy(gv.at[span], gv_hbm.at[span], out_sem.at[0, j]),
            pltpu.make_async_copy(gg.at[span], gg_hbm.at[span], out_sem.at[1, j]),
        ]

    outs = []

    def write(copies):
        for c in copies:
            c.start()
            outs.append(c)

    write(gated_gradient(0))

    to_pair.wait()
    small_all[chip] = small[pl.ds(par * half, half)] + small_in[...]

    def all_copy(i):
        return remote(
            small_all.at[chip], small_all.at[chip], sa_s.at[i], sa_r.at[i],
            {"sp": lax.rem(chip + i, nc) * 2 + par},
        )

    @pl.loop(1, nc)
    def _(i):
        all_copy(i).start()

    for j in range(1, chunks - 1):
        write(gated_gradient(j))

    back.wait()
    last = me == n - 1
    for cb in range(blocks):
        h = back_in[cb]
        gcpad[cb, pl.ds(rows, HALO), :] = jnp.where(last, jnp.zeros_like(h), h)
    write(gated_gradient(chunks - 1))

    pair_copy(0).wait()
    gp[...] = full[me] + pair_in[0].astype(F32)

    @pl.loop(1, nc)
    def _(i):
        ring_copy(i).wait()
        gp[...] += ring_in[i].astype(F32)

    write([pltpu.make_async_copy(gp, gp_hbm, out_sem.at[2, 0])])

    @pl.loop(1, nc)
    def _(i):
        all_copy(i).wait()

    small_tot[...] = small_all[0]

    @pl.loop(1, nc)
    def _(i):
        small_tot[...] += small_all[i]

    fin = remote(small_tot, small_fin, sf_sem.at[0], sf_sem.at[1], {"sp": partner})
    fin.start()
    write([
        pltpu.make_async_copy(
            small_tot, small_hbm.at[pl.ds(par * half, half)], out_sem.at[2, 1]
        )
    ])
    fin.wait()
    write([
        pltpu.make_async_copy(
            small_fin, small_hbm.at[pl.ds((1 - par) * half, half)], out_sem.at[2, 2]
        )
    ])
    for c in outs:
        c.wait()


def on_device(n, tp, value, gate, taps, gain, bias, proj, grad):
    rows, width = value.shape
    model = grad.shape[1]
    taps_n = taps.shape[0]
    blocks = width // LANES
    chunks = rows // LANES
    nc = n // 2
    half = blocks // 2
    share = model // n
    any_spec = pl.BlockSpec(memory_space=pl.ANY)
    vmem = pl.BlockSpec(memory_space=pltpu.VMEM)
    sem = pltpu.SemaphoreType.DMA
    wide = pltpu.VMEM((blocks, rows, LANES), F32)
    padded = pltpu.VMEM((blocks, rows + HALO, LANES), F32)
    gv, gg, small, gp = pl.pallas_call(
        functools.partial(kernel, n, tp, taps_n),
        out_shape=(
            jax.ShapeDtypeStruct((rows, width), BF16),
            jax.ShapeDtypeStruct((rows, width), BF16),
            jax.ShapeDtypeStruct((blocks, SMALL, LANES), F32),
            jax.ShapeDtypeStruct((share, width), F32),
        ),
        in_specs=[any_spec, any_spec, vmem, vmem, vmem, any_spec, any_spec],
        out_specs=(any_spec,) * 4,
        scratch_shapes=[
            pltpu.VMEM((rows, width), BF16),
            pltpu.VMEM((rows, width), BF16),
            pltpu.VMEM((width, model), BF16),
            pltpu.VMEM((rows, model), BF16),
            padded, wide, wide, wide, padded,
            pltpu.VMEM((rows, width), BF16),
            pltpu.VMEM((n, share, width), F32),
            pltpu.VMEM((nc, share, width), BF16),
            pltpu.VMEM((nc, share, width), BF16),
            pltpu.VMEM((nc, share, width), BF16),
            pltpu.VMEM((nc, share, width), BF16),
            pltpu.VMEM((blocks, HALO, LANES), BF16),
            pltpu.VMEM((blocks, HALO, LANES), BF16),
            pltpu.VMEM((blocks, HALO, LANES), F32),
            pltpu.VMEM((blocks, HALO, LANES), F32),
            pltpu.VMEM((2, LANES, LANES), F32),
            pltpu.VMEM((LANES, LANES), F32),
            pltpu.VMEM((rows, LANES), F32),
            pltpu.VMEM((chunks, 8, LANES), F32),
            pltpu.VMEM((chunks, tp - 1, 8, LANES), F32),
            pltpu.VMEM((chunks, 8, LANES), F32),
            pltpu.VMEM((chunks, tp - 1, 8, LANES), F32),
            pltpu.VMEM((blocks, taps_n + 2, 8, LANES), F32),
            pltpu.VMEM((blocks, SMALL, LANES), F32),
            pltpu.VMEM((half, SMALL, LANES), F32),
            pltpu.VMEM((nc, half, SMALL, LANES), F32),
            pltpu.VMEM((half, SMALL, LANES), F32),
            pltpu.VMEM((half, SMALL, LANES), F32),
            pltpu.VMEM((rows, width), BF16),
            pltpu.VMEM((rows, width), BF16),
            pltpu.VMEM((share, width), F32),
            sem((4,)), sem((3, max(chunks, 3))), sem((2,)), sem((2,)),
            sem((2, chunks, tp - 1)), sem((2, chunks, tp - 1)),
            sem((nc,)), sem((nc,)), sem((nc,)), sem((nc,)),
            sem((2,)), sem((nc,)), sem((nc,)), sem((2,)),
        ],
        compiler_params=pltpu.CompilerParams(
            collective_id=0, has_side_effects=True, vmem_limit_bytes=60 * 1024 * 1024
        ),
    )(value, gate, taps, gain.reshape(1, width), bias.reshape(1, width), proj, grad)
    small = small.transpose(1, 0, 2).reshape(SMALL, width)
    return gv, gg, small[:taps_n], small[taps_n], small[taps_n + 1], gp


def solution(mesh):
    n, tp = mesh.shape["sp"], mesh.shape["tp"]
    return jax.shard_map(
        functools.partial(on_device, n, tp),
        mesh=mesh,
        in_specs=(
            P("sp", "tp"),
            P("sp", "tp"),
            P(None, "tp"),
            P("tp"),
            P("tp"),
            P("tp", None),
            P("sp", None),
        ),
        out_specs=(P("sp", "tp"), P("sp", "tp"), P(None, "tp"), P("tp"), P("tp"), P("sp", "tp")),
        check_vma=False,
    )
```

```python
import functools

import jax
import jax.numpy as jnp
from jax import lax
from jax.experimental import pallas as pl
from jax.experimental.pallas import tpu as pltpu
from jax.sharding import PartitionSpec as P

LANES = 128
HALO = 32
SMALL = 40
MESH = pl.DeviceIdType.MESH
F32, BF16 = jnp.float32, jnp.bfloat16


def kernel(
    n, tp, taps_n, ysize,
    value_hbm, gate_hbm, taps_ref, gain_ref, bias_ref, proj_hbm, grad_hbm,
    gv, gg, gp, taps_out, gain_out, bias_out,
    value, gate, proj, grad, gpad, conv, gact, gnorm, gcpad, act,
    grad_t, full, pair_out, pair_in, y_out, y_in, z_out, z_in,
    halo_out, halo_in, back_out, back_in,
    stage, mean_b, rstd_b, stat_out, stat_in, stat2_out, stat2_in,
    tacc, small, small_in, small_y, small_z, small_fin, small_tot,
    in_sem, halo_sem, back_sem, stat_sem, stat2_sem,
    pair_sem, y_sem, z_sem, sp_sem, sy_sem, sz_sem, sf_sem,
):
    rows, width = value.shape
    blocks = width // LANES
    chunks = rows // LANES
    nc = n // 2
    half = blocks // 2
    share = full.shape[1]
    model = grad.shape[1]
    channels = width * tp
    me = lax.axis_index("sp")
    col = lax.axis_index("tp")
    par = lax.rem(me, 2)
    chip = me // 2
    partner = chip * 2 + 1 - par
    zsize = nc // ysize
    cy = lax.rem(chip, ysize)
    cz = chip // ysize
    zorder = list(range(zsize // 2, zsize)) + list(range(1, zsize // 2)) + [0]
    nxt = lax.rem(me + 1, n)
    prv = lax.rem(me + n - 1, n)

    loads = [
        pltpu.make_async_copy(s, d, in_sem.at[i])
        for i, (s, d) in enumerate(
            ((value_hbm, value), (gate_hbm, gate), (grad_hbm, grad), (proj_hbm, proj))
        )
    ]
    for c in loads:
        c.start()

    barrier = pltpu.get_barrier_semaphore()

    @pl.loop(1, n)
    def _(i):
        pl.semaphore_signal(
            barrier, inc=1, device_id={"sp": lax.rem(me + i, n)}, device_id_type=MESH
        )

    for t in range(1, tp):
        pl.semaphore_signal(
            barrier, inc=1, device_id={"tp": lax.rem(col + t, tp)}, device_id_type=MESH
        )

    def remote(src, dst, s, r, where):
        return pltpu.make_async_remote_copy(
            src_ref=src, dst_ref=dst, send_sem=s, recv_sem=r,
            device_id=where, device_id_type=MESH,
        )

    def lanes(cb):
        return pl.ds(pl.multiple_of(cb * LANES, LANES), LANES)

    def stat_copy(out, inn, sem, j, t):
        return remote(
            out.at[j], inn.at[j, t - 1], sem.at[0, j, t - 1], sem.at[1, j, t - 1],
            {"tp": lax.rem(col + t, tp)},
        )

    sub = lax.broadcasted_iota(jnp.int32, (8, LANES), 0)

    def send_stats(out, inn, sem, j):
        a = jnp.sum(stage[0].T, axis=0, keepdims=True)
        b = jnp.sum(stage[1].T, axis=0, keepdims=True)
        out[j] = jnp.where(sub == 0, a, b)
        for t in range(1, tp):
            stat_copy(out, inn, sem, j, t).start()

    def recv_stats(out, inn, sem, j):
        total = out[j]
        for t in range(1, tp):
            stat_copy(out, inn, sem, j, t).wait()
            total = total + inn[j, t - 1]
        total = total / channels
        return total[0:1], total[1:2]

    loads[0].wait()
    loads[1].wait()

    def gated_rows(r0, cb, count):
        v = value[pl.ds(r0, count), lanes(cb)].astype(F32)
        s = jax.nn.sigmoid(gate[pl.ds(r0, count), lanes(cb)].astype(F32))
        return (v * s).astype(BF16)

    for cb in range(blocks):
        g = gated_rows(rows - HALO, cb, HALO)
        halo_out[cb] = g
    pl.semaphore_wait(barrier, n - 1 + tp - 1)
    halo = remote(halo_out, halo_in, halo_sem.at[0], halo_sem.at[1], {"sp": nxt})
    halo.start()

    @pl.loop(0, rows // 64)
    def _(i):
        r0 = pl.multiple_of(i * 64, 64)
        for cb in range(blocks):
            gpad[cb, pl.ds(r0 + HALO, 64), :] = gated_rows(r0, cb, 64).astype(F32)

    def tap_row(k, cb):
        return taps_ref[pl.ds(k, 1), lanes(cb)]

    def conv_chunk(j):
        for h in range(LANES // 64):
            r0 = j * LANES + h * 64

            def body(cb, carry):
                s, q = carry
                acc = tap_row(0, cb) * gpad[cb, pl.ds(r0 + 2, 64), :]
                for k in range(1, taps_n):
                    acc = acc + tap_row(k, cb) * gpad[cb, pl.ds(r0 + HALO - taps_n + 1 + k, 64), :]
                conv[cb, pl.ds(r0, 64), :] = acc
                step = (j * (LANES // 64) + h) * blocks + cb
                for e in range(per_step):
                    tile = step * per_step + e
                    across = pl.ds(pl.multiple_of(tile % chunks * LANES, LANES), LANES)
                    down = pl.ds(pl.multiple_of(tile // chunks * LANES, LANES), LANES)
                    grad_t[down, across] = grad[across, down].T
                return s + acc, q + acc * acc

            zero = jnp.zeros((64, LANES), F32)
            s, q = lax.fori_loop(0, blocks, body, (zero, zero))
            stage[0, pl.ds(h * 64, 64), :] = s
            stage[1, pl.ds(h * 64, 64), :] = q
        send_stats(stat_out, stat_in, stat_sem, j)

    order = list(range(1, chunks)) + [0]
    per_step = (model // LANES) * chunks // (chunks * (LANES // 64) * blocks)
    loads[2].wait()
    for j in order:
        if j == 0:
            halo.wait()
            first = me == 0
            for cb in range(blocks):
                h = halo_in[cb].astype(F32)
                gpad[cb, pl.ds(0, HALO), :] = jnp.where(first, jnp.zeros_like(h), h)
        conv_chunk(j)

    loads[3].wait()
    for cb in range(0, blocks, 2):
        both = lax.dot_general(
            grad[...], proj[pl.ds(cb * LANES, 2 * LANES), :], (((1,), (1,)), ((), ())),
            preferred_element_type=F32,
        )
        gact[cb] = both[:, :LANES]
        gact[cb + 1] = both[:, LANES:]

    tacc[...] = jnp.zeros_like(tacc)

    def norm_chunk(j):
        mean, sq = recv_stats(stat_out, stat_in, stat_sem, j)
        rstd = lax.rsqrt(sq - mean * mean + 1e-05)
        mean_b[...] = jnp.broadcast_to(mean, (LANES, LANES)).T
        rstd_b[pl.ds(j * LANES, LANES), :] = jnp.broadcast_to(rstd, (LANES, LANES)).T

        @pl.loop(0, LANES // 32)
        def _(h):
            l0 = pl.multiple_of(h * 32, 32)
            r0 = pl.multiple_of(j * LANES + l0, 32)
            m = mean_b[pl.ds(l0, 32), :]
            rs = rstd_b[pl.ds(r0, 32), :]
            s1 = jnp.zeros((32, LANES), F32)
            s2 = jnp.zeros((32, LANES), F32)
            for cb in range(blocks):
                cols = pl.ds(cb * LANES, LANES)
                gain = gain_ref[:, cols]
                xhat = (conv[cb, pl.ds(r0, 32), :] - m) * rs
                nrm = xhat * gain + bias_ref[:, cols]
                sig = jax.nn.sigmoid(nrm)
                act[pl.ds(r0, 32), cols] = (nrm * sig).astype(BF16)
                gn = gact[cb, pl.ds(r0, 32), :] * sig * (1.0 + nrm * (1.0 - sig))
                conv[cb, pl.ds(r0, 32), :] = xhat
                gx = gn * gain
                gnorm[cb, pl.ds(r0, 32), :] = gx
                gxx = gx * xhat
                s1 = s1 + gx
                s2 = s2 + gxx
                tacc[cb, taps_n] += jnp.sum((gn * xhat).reshape(4, 8, LANES), axis=0)
                tacc[cb, taps_n + 1] += jnp.sum(gn.reshape(4, 8, LANES), axis=0)
            stage[0, pl.ds(l0, 32), :] = s1
            stage[1, pl.ds(l0, 32), :] = s2

        send_stats(stat2_out, stat2_in, stat2_sem, j)

    for j in order:
        norm_chunk(j)

    def owners(k):
        return lax.rem(cz + zorder[k], zsize) * 2 * ysize

    def pair_copy(k):
        return remote(
            pair_out.at[k], pair_in.at[k], pair_sem.at[0, k], pair_sem.at[1, k],
            {"sp": partner},
        )

    def y_copy(k, i):
        return remote(
            y_out.at[k, i - 1], y_in.at[k, i - 1], y_sem.at[0, k, i - 1],
            y_sem.at[1, k, i - 1],
            {"sp": (cz * ysize + lax.rem(cy + i, ysize)) * 2 + par},
        )

    def z_copy(k):
        return remote(
            z_out.at[k], z_in.at[k], z_sem.at[0, k], z_sem.at[1, k],
            {"sp": (lax.rem(cz + zorder[k], zsize) * ysize + cy) * 2 + par},
        )

    def pair_stage(k):
        base = owners(k)
        span = 2 * ysize * share
        part = lax.dot_general(
            grad_t[pl.ds(pl.multiple_of(base * share, LANES), span), :], act[...],
            (((1,), (0,)), ((), ())), preferred_element_type=F32,
        )
        full[pl.ds(base, 2 * ysize)] = part.reshape(2 * ysize, share, width)
        for y in range(ysize):
            pair_out[k, y] = full[base + 2 * y + 1 - par].astype(BF16)
        pair_copy(k).start()

    def y_stage(k):
        base = owners(k)
        pair_copy(k).wait()
        for i in range(1, ysize):
            y = lax.rem(cy + i, ysize)
            y_out[k, i - 1] = (full[base + 2 * y + par] + pair_in[k, y].astype(F32)).astype(BF16)
            y_copy(k, i).start()

    def z_stage(k):
        acc = full[owners(k) + 2 * cy + par] + pair_in[k, cy].astype(F32)
        for i in range(1, ysize):
            y_copy(k, i).wait()
            acc = acc + y_in[k, i - 1].astype(F32)
        if zorder[k]:
            z_out[k] = acc.astype(BF16)
            z_copy(k).start()
        else:
            gp[...] = acc

    def gconv_chunk(j):
        m1, m2 = recv_stats(stat2_out, stat2_in, stat2_sem, j)
        stage[0] = jnp.broadcast_to(m1, (LANES, LANES)).T
        stage[1] = jnp.broadcast_to(m2, (LANES, LANES)).T

        @pl.loop(0, LANES // 64)
        def _(h):
            l0 = pl.multiple_of(h * 64, 64)
            r0 = pl.multiple_of(j * LANES + l0, 64)
            a = stage[0, pl.ds(l0, 64), :]
            b = stage[1, pl.ds(l0, 64), :]
            rs = rstd_b[pl.ds(r0, 64), :]
            for cb in range(blocks):
                gcpad[cb, pl.ds(r0, 64), :] = rs * (
                    gnorm[cb, pl.ds(r0, 64), :] - a - conv[cb, pl.ds(r0, 64), :] * b
                )

    def send_back():
        gconv_chunk(0)
        for cb in range(blocks):
            back_out[cb] = gcpad[cb, pl.ds(0, HALO), :]
        back.start()

    back = remote(back_out, back_in, back_sem.at[0], back_sem.at[1], {"sp": prv})

    def taps_rows(first, count):
        @pl.loop(first, first + count)
        def _(i):
            r0 = pl.multiple_of(i * 64, 64)

            @pl.loop(0, blocks)
            def _(cb):
                gc = gcpad[cb, pl.ds(r0, 64), :]
                for k in range(taps_n):
                    prod = gc * gpad[cb, pl.ds(r0 + HALO - taps_n + 1 + k, 64), :]
                    tacc[cb, k] += jnp.sum(prod.reshape(8, 8, LANES), axis=0)

    for k in range(zsize):
        pair_stage(k)
        if k == 1:
            send_back()
        if k >= 1:
            y_stage(k - 1)
    for j in range(1, chunks):
        gconv_chunk(j)

    steps = rows // 64
    taps_rows(0, steps // 2)
    z_stage(0)
    taps_rows(steps // 2, steps - steps // 2)

    small[...] = jnp.zeros_like(small)
    for cb in range(blocks):
        small[cb, pl.ds(0, taps_n + 2), :] = jnp.sum(tacc[cb], axis=1)
    to_pair = remote(
        small.at[pl.ds((1 - par) * half, half)], small_in, sp_sem.at[0], sp_sem.at[1],
        {"sp": partner},
    )
    to_pair.start()

    def gated_gradient(j):
        @pl.loop(0, LANES // 64)
        def _(h):
            r0 = pl.multiple_of(j * LANES + h * 64, 64)

            @pl.loop(0, blocks)
            def _(cb):
                acc = tap_row(0, cb) * gcpad[cb, pl.ds(r0 + taps_n - 1, 64), :]
                for k in range(1, taps_n):
                    acc = acc + tap_row(k, cb) * gcpad[cb, pl.ds(r0 + taps_n - 1 - k, 64), :]
                v = value[pl.ds(r0, 64), lanes(cb)].astype(F32)
                s = jax.nn.sigmoid(gate[pl.ds(r0, 64), lanes(cb)].astype(F32))
                ds = acc * s
                gv[pl.ds(r0, 64), lanes(cb)] = ds.astype(BF16)
                gg[pl.ds(r0, 64), lanes(cb)] = (ds * v * (1.0 - s)).astype(BF16)

    z_stage(1)
    to_pair.wait()
    small_y[cy] = small[pl.ds(par * half, half)] + small_in[...]

    def small_y_copy(i):
        return remote(
            small_y.at[cy], small_y.at[cy], sy_sem.at[0, i - 1], sy_sem.at[1, i - 1],
            {"sp": (cz * ysize + lax.rem(cy + i, ysize)) * 2 + par},
        )

    def small_z_copy(i):
        return remote(
            small_z.at[cz], small_z.at[cz], sz_sem.at[0, i - 1], sz_sem.at[1, i - 1],
            {"sp": (lax.rem(cz + i, zsize) * ysize + cy) * 2 + par},
        )

    for i in range(1, ysize):
        small_y_copy(i).start()
    y_stage(zsize - 1)

    gated_gradient(0)
    for k in range(2, zsize - 1):
        z_stage(k)
    gated_gradient(1)

    for i in range(1, ysize):
        small_y_copy(i).wait()
    total = small_y[0]
    for i in range(1, ysize):
        total = total + small_y[i]
    small_z[cz] = total
    for i in range(1, zsize):
        small_z_copy(i).start()

    for j in range(2, chunks - 1):
        gated_gradient(j)

    back.wait()
    last = me == n - 1
    for cb in range(blocks):
        h = back_in[cb]
        gcpad[cb, pl.ds(rows, HALO), :] = jnp.where(last, jnp.zeros_like(h), h)
    gated_gradient(chunks - 1)

    z_stage(zsize - 1)
    for i in range(1, zsize):
        small_z_copy(i).wait()
    total = small_z[0]
    for i in range(1, zsize):
        total = total + small_z[i]
    small_tot[...] = total
    fin = remote(small_tot, small_fin, sf_sem.at[0], sf_sem.at[1], {"sp": partner})
    fin.start()

    for k in range(zsize - 1):
        z_copy(k).wait()
        gp[...] += z_in[k].astype(F32)

    fin.wait()
    for cb in range(half):
        for source, where in ((small_tot, par), (small_fin, 1 - par)):
            cols = lanes(where * half + cb)
            taps_out[:, cols] = source[cb, pl.ds(0, taps_n), :]
            gain_out[:, cols] = source[cb, pl.ds(taps_n, 1), :]
            bias_out[:, cols] = source[cb, pl.ds(taps_n + 1, 1), :]


def on_device(n, tp, value, gate, taps, gain, bias, proj, grad):
    rows, width = value.shape
    model = grad.shape[1]
    taps_n = taps.shape[0]
    blocks = width // LANES
    chunks = rows // LANES
    nc = n // 2
    half = blocks // 2
    share = model // n
    ysize = 1
    while 2 * (2 * ysize) ** 2 <= nc:
        ysize *= 2
    zsize = nc // ysize
    hbm = pl.BlockSpec(memory_space=pltpu.HBM)
    vmem = pl.BlockSpec(memory_space=pltpu.VMEM)
    sem = pltpu.SemaphoreType.DMA
    wide = pltpu.VMEM((blocks, rows, LANES), F32)
    padded = pltpu.VMEM((blocks, rows + HALO, LANES), F32)
    gv, gg, gp, dtaps, dgain, dbias = pl.pallas_call(
        functools.partial(kernel, n, tp, taps_n, ysize),
        out_shape=(
            jax.ShapeDtypeStruct((rows, width), BF16),
            jax.ShapeDtypeStruct((rows, width), BF16),
            jax.ShapeDtypeStruct((share, width), F32),
            jax.ShapeDtypeStruct((taps_n, width), F32),
            jax.ShapeDtypeStruct((1, width), F32),
            jax.ShapeDtypeStruct((1, width), F32),
        ),
        in_specs=[hbm, hbm, vmem, vmem, vmem, hbm, hbm],
        out_specs=(vmem,) * 6,
        scratch_shapes=[
            pltpu.VMEM((rows, width), BF16),
            pltpu.VMEM((rows, width), BF16),
            pltpu.VMEM((width, model), BF16),
            pltpu.VMEM((rows, model), BF16),
            padded, wide, wide, wide, padded,
            pltpu.VMEM((rows, width), BF16),
            pltpu.VMEM((model, rows), BF16),
            pltpu.VMEM((n, share, width), F32),
            pltpu.VMEM((zsize, ysize, share, width), BF16),
            pltpu.VMEM((zsize, ysize, share, width), BF16),
            pltpu.VMEM((zsize, ysize - 1, share, width), BF16),
            pltpu.VMEM((zsize, ysize - 1, share, width), BF16),
            pltpu.VMEM((zsize - 1, share, width), BF16),
            pltpu.VMEM((zsize - 1, share, width), BF16),
            pltpu.VMEM((blocks, HALO, LANES), BF16),
            pltpu.VMEM((blocks, HALO, LANES), BF16),
            pltpu.VMEM((blocks, HALO, LANES), F32),
            pltpu.VMEM((blocks, HALO, LANES), F32),
            pltpu.VMEM((2, LANES, LANES), F32),
            pltpu.VMEM((LANES, LANES), F32),
            pltpu.VMEM((rows, LANES), F32),
            pltpu.VMEM((chunks, 8, LANES), F32),
            pltpu.VMEM((chunks, tp - 1, 8, LANES), F32),
            pltpu.VMEM((chunks, 8, LANES), F32),
            pltpu.VMEM((chunks, tp - 1, 8, LANES), F32),
            pltpu.VMEM((blocks, taps_n + 2, 8, LANES), F32),
            pltpu.VMEM((blocks, SMALL, LANES), F32),
            pltpu.VMEM((half, SMALL, LANES), F32),
            pltpu.VMEM((ysize, half, SMALL, LANES), F32),
            pltpu.VMEM((zsize, half, SMALL, LANES), F32),
            pltpu.VMEM((half, SMALL, LANES), F32),
            pltpu.VMEM((half, SMALL, LANES), F32),
            sem((4,)), sem((2,)), sem((2,)),
            sem((2, chunks, tp - 1)), sem((2, chunks, tp - 1)),
            sem((2, zsize)), sem((2, zsize, ysize - 1)), sem((2, zsize - 1)),
            sem((2,)), sem((2, ysize - 1)), sem((2, zsize - 1)), sem((2,)),
        ],
        compiler_params=pltpu.CompilerParams(
            collective_id=0, has_side_effects=True, vmem_limit_bytes=36 * 1024 * 1024
        ),
    )(value, gate, taps, gain.reshape(1, width), bias.reshape(1, width), proj, grad)
    return gv, gg, dtaps, dgain.reshape(width), dbias.reshape(width), gp


def solution(mesh):
    n, tp = mesh.shape["sp"], mesh.shape["tp"]
    return jax.shard_map(
        functools.partial(on_device, n, tp),
        mesh=mesh,
        in_specs=(
            P("sp", "tp"),
            P("sp", "tp"),
            P(None, "tp"),
            P("tp"),
            P("tp"),
            P("tp", None),
            P("sp", None),
        ),
        out_specs=(P("sp", "tp"), P("sp", "tp"), P(None, "tp"), P("tp"), P("tp"), P("sp", "tp")),
        check_vma=False,
    )
```

```python
import functools

import jax
import jax.numpy as jnp
from jax import lax
from jax.experimental import pallas as pl
from jax.experimental.pallas import tpu as pltpu
from jax.sharding import PartitionSpec as P

LANES = 128
HALO = 32
SMALL = 40
MESH = pl.DeviceIdType.MESH
F32, BF16 = jnp.float32, jnp.bfloat16


def kernel(
    n, tp, taps_n, ysize,
    value_hbm, gate_hbm, taps_hbm, gain_hbm, bias_hbm, proj_hbm, grad_hbm,
    gv, gg, gp, taps_out, gain_out, bias_out,
    value, gate, taps_ref, gain_ref, bias_ref, proj, grad, gpad, conv, gact, gnorm, gcpad, act,
    grad_t, full, pair_out, pair_in, y_out, y_in, z_out, z_in,
    halo_out, halo_in, back_out, back_in,
    stage, mean_b, rstd_b, stat_out, stat_in, stat2_out, stat2_in,
    tacc, small, small_in, small_y, small_z, small_zin, small_fin, small_tot,
    in_sem, halo_sem, back_sem, stat_sem, stat2_sem,
    pair_sem, y_sem, z_sem, sp_sem, sy_sem, sz_sem, sf_sem,
):
    rows, width = value.shape
    blocks = width // LANES
    chunks = rows // LANES
    nc = n // 2
    half = blocks // 2
    share = full.shape[1]
    model = grad.shape[1]
    channels = width * tp
    me = lax.axis_index("sp")
    col = lax.axis_index("tp")
    par = lax.rem(me, 2)
    chip = me // 2
    partner = chip * 2 + 1 - par
    zsize = nc // ysize
    cy = lax.rem(chip, ysize)
    cz = chip // ysize
    zorder = list(range(zsize // 2, zsize)) + list(range(1, zsize // 2)) + [0]
    nxt = lax.rem(me + 1, n)
    prv = lax.rem(me + n - 1, n)

    loads = [
        pltpu.make_async_copy(s, d, in_sem.at[i])
        for i, (s, d) in enumerate(
            (
                (value_hbm, value), (gate_hbm, gate), (grad_hbm, grad), (proj_hbm, proj),
                (taps_hbm, taps_ref), (gain_hbm, gain_ref), (bias_hbm, bias_ref),
            )
        )
    ]
    for i in (0, 1, 4, 2, 3, 5, 6):
        loads[i].start()

    barrier = pltpu.get_barrier_semaphore()

    @pl.loop(1, n)
    def _(i):
        pl.semaphore_signal(
            barrier, inc=1, device_id={"sp": lax.rem(me + i, n)}, device_id_type=MESH
        )

    for t in range(1, tp):
        pl.semaphore_signal(
            barrier, inc=1, device_id={"tp": lax.rem(col + t, tp)}, device_id_type=MESH
        )

    def remote(src, dst, s, r, where):
        return pltpu.make_async_remote_copy(
            src_ref=src, dst_ref=dst, send_sem=s, recv_sem=r,
            device_id=where, device_id_type=MESH,
        )

    def lanes(cb):
        return pl.ds(pl.multiple_of(cb * LANES, LANES), LANES)

    def stat_copy(out, inn, sem, j, t):
        return remote(
            out.at[j], inn.at[j, t - 1], sem.at[0, j, t - 1], sem.at[1, j, t - 1],
            {"tp": lax.rem(col + t, tp)},
        )

    sub = lax.broadcasted_iota(jnp.int32, (8, LANES), 0)

    def send_stats(out, inn, sem, j):
        a = jnp.sum(stage[0].T, axis=0, keepdims=True)
        b = jnp.sum(stage[1].T, axis=0, keepdims=True)
        out[j] = jnp.where(sub == 0, a, b)
        for t in range(1, tp):
            stat_copy(out, inn, sem, j, t).start()

    def recv_stats(out, inn, sem, j):
        total = out[j]
        for t in range(1, tp):
            stat_copy(out, inn, sem, j, t).wait()
            total = total + inn[j, t - 1]
        total = total / channels
        return total[0:1], total[1:2]

    loads[0].wait()
    loads[1].wait()

    def gated_rows(r0, cb, count):
        v = value[pl.ds(r0, count), lanes(cb)].astype(F32)
        s = jax.nn.sigmoid(gate[pl.ds(r0, count), lanes(cb)].astype(F32))
        return (v * s).astype(BF16)

    for cb in range(blocks):
        g = gated_rows(rows - HALO, cb, HALO)
        halo_out[cb] = g
    halo = remote(halo_out, halo_in, halo_sem.at[0], halo_sem.at[1], {"sp": nxt})

    @pl.loop(0, rows // 64)
    def _(i):
        r0 = pl.multiple_of(i * 64, 64)
        for cb in range(blocks):
            gpad[cb, pl.ds(r0 + HALO, 64), :] = gated_rows(r0, cb, 64).astype(F32)

    def tap_row(k, cb):
        return taps_ref[pl.ds(k, 1), lanes(cb)]

    def conv_chunk(j):
        for h in range(LANES // 64):
            r0 = j * LANES + h * 64

            def body(cb, carry):
                s, q = carry
                step = (j * (LANES // 64) + h) * blocks + cb
                tiles = []
                for e in range(per_step):
                    tile = step * per_step + e
                    across = pl.ds(pl.multiple_of(tile % chunks * LANES, LANES), LANES)
                    down = pl.ds(pl.multiple_of(tile // chunks * LANES, LANES), LANES)
                    tiles.append((down, across, grad[across, down].T))
                acc = tap_row(0, cb) * gpad[cb, pl.ds(r0 + 2, 64), :]
                for k in range(1, taps_n):
                    acc = acc + tap_row(k, cb) * gpad[cb, pl.ds(r0 + HALO - taps_n + 1 + k, 64), :]
                conv[cb, pl.ds(r0, 64), :] = acc
                for down, across, tile in tiles:
                    grad_t[down, across] = tile
                return s + acc, q + acc * acc

            zero = jnp.zeros((64, LANES), F32)
            s, q = lax.fori_loop(0, blocks, body, (zero, zero))
            stage[0, pl.ds(h * 64, 64), :] = s
            stage[1, pl.ds(h * 64, 64), :] = q
        if j == 1:
            pl.semaphore_wait(barrier, n - 1 + tp - 1)
            halo.start()
        send_stats(stat_out, stat_in, stat_sem, j)

    order = list(range(1, chunks)) + [0]
    per_step = (model // LANES) * chunks // (chunks * (LANES // 64) * blocks)
    loads[4].wait()
    loads[2].wait()
    for j in order:
        if j == 0:
            halo.wait()
            first = me == 0
            for cb in range(blocks):
                h = halo_in[cb].astype(F32)
                gpad[cb, pl.ds(0, HALO), :] = jnp.where(first, jnp.zeros_like(h), h)
        conv_chunk(j)

    loads[3].wait()
    loads[5].wait()
    loads[6].wait()
    for cb in range(0, blocks, 2):
        both = lax.dot_general(
            grad[...], proj[pl.ds(cb * LANES, 2 * LANES), :], (((1,), (1,)), ((), ())),
            preferred_element_type=F32,
        )
        gact[cb] = both[:, :LANES]
        gact[cb + 1] = both[:, LANES:]

    tacc[...] = jnp.zeros_like(tacc)

    def norm_chunk(j):
        mean, sq = recv_stats(stat_out, stat_in, stat_sem, j)
        rstd = lax.rsqrt(sq - mean * mean + 1e-05)
        mean_b[...] = jnp.broadcast_to(mean, (LANES, LANES)).T
        rstd_b[pl.ds(j * LANES, LANES), :] = jnp.broadcast_to(rstd, (LANES, LANES)).T

        @pl.loop(0, LANES // 32)
        def _(h):
            l0 = pl.multiple_of(h * 32, 32)
            r0 = pl.multiple_of(j * LANES + l0, 32)
            m = mean_b[pl.ds(l0, 32), :]
            rs = rstd_b[pl.ds(r0, 32), :]
            s1 = jnp.zeros((32, LANES), F32)
            s2 = jnp.zeros((32, LANES), F32)
            for cb in range(blocks):
                cols = pl.ds(cb * LANES, LANES)
                gain = gain_ref[:, cols]
                xhat = (conv[cb, pl.ds(r0, 32), :] - m) * rs
                nrm = xhat * gain + bias_ref[:, cols]
                sig = jax.nn.sigmoid(nrm)
                act[pl.ds(r0, 32), cols] = (nrm * sig).astype(BF16)
                gn = gact[cb, pl.ds(r0, 32), :] * sig * (1.0 + nrm * (1.0 - sig))
                conv[cb, pl.ds(r0, 32), :] = xhat
                gx = gn * gain
                gnorm[cb, pl.ds(r0, 32), :] = gx
                gxx = gx * xhat
                s1 = s1 + gx
                s2 = s2 + gxx
                tacc[cb, taps_n] += jnp.sum((gn * xhat).reshape(4, 8, LANES), axis=0)
                tacc[cb, taps_n + 1] += jnp.sum(gn.reshape(4, 8, LANES), axis=0)
            stage[0, pl.ds(l0, 32), :] = s1
            stage[1, pl.ds(l0, 32), :] = s2

        send_stats(stat2_out, stat2_in, stat2_sem, j)

    for j in order:
        norm_chunk(j)

    def owners(k):
        return lax.rem(cz + zorder[k], zsize) * 2 * ysize

    def pair_copy(k):
        return remote(
            pair_out.at[k], pair_in.at[k], pair_sem.at[0, k], pair_sem.at[1, k],
            {"sp": partner},
        )

    def y_copy(k, i):
        return remote(
            y_out.at[k, i - 1], y_in.at[k, i - 1], y_sem.at[0, k, i - 1],
            y_sem.at[1, k, i - 1],
            {"sp": (cz * ysize + lax.rem(cy + i, ysize)) * 2 + par},
        )

    def z_copy(k):
        return remote(
            z_out.at[k], z_in.at[k], z_sem.at[0, k], z_sem.at[1, k],
            {"sp": (lax.rem(cz + zorder[k], zsize) * ysize + cy) * 2 + par},
        )

    def pair_stage(k):
        base = owners(k)
        span = 2 * ysize * share
        part = lax.dot_general(
            grad_t[pl.ds(pl.multiple_of(base * share, LANES), span), :], act[...],
            (((1,), (0,)), ((), ())), preferred_element_type=F32,
        )
        full[pl.ds(base, 2 * ysize)] = part.reshape(2 * ysize, share, width)
        for y in range(ysize):
            pair_out[k, y] = full[base + 2 * y + 1 - par].astype(BF16)
        pair_copy(k).start()

    def y_stage(k):
        base = owners(k)
        pair_copy(k).wait()
        for i in range(1, ysize):
            y = lax.rem(cy + i, ysize)
            y_out[k, i - 1] = (full[base + 2 * y + par] + pair_in[k, y].astype(F32)).astype(BF16)
            y_copy(k, i).start()

    def z_stage(k):
        acc = full[owners(k) + 2 * cy + par] + pair_in[k, cy].astype(F32)
        for i in range(1, ysize):
            y_copy(k, i).wait()
            acc = acc + y_in[k, i - 1].astype(F32)
        if zorder[k]:
            z_out[k] = acc.astype(BF16)
            z_copy(k).start()
        else:
            gp[...] = acc

    def gconv_chunk(j):
        m1, m2 = recv_stats(stat2_out, stat2_in, stat2_sem, j)
        stage[0] = jnp.broadcast_to(m1, (LANES, LANES)).T
        stage[1] = jnp.broadcast_to(m2, (LANES, LANES)).T

        @pl.loop(0, LANES // 64)
        def _(h):
            l0 = pl.multiple_of(h * 64, 64)
            r0 = pl.multiple_of(j * LANES + l0, 64)
            a = stage[0, pl.ds(l0, 64), :]
            b = stage[1, pl.ds(l0, 64), :]
            rs = rstd_b[pl.ds(r0, 64), :]
            for cb in range(blocks):
                gcpad[cb, pl.ds(r0, 64), :] = rs * (
                    gnorm[cb, pl.ds(r0, 64), :] - a - conv[cb, pl.ds(r0, 64), :] * b
                )

    def send_back():
        gconv_chunk(0)
        for cb in range(blocks):
            back_out[cb] = gcpad[cb, pl.ds(0, HALO), :]
        back.start()

    back = remote(back_out, back_in, back_sem.at[0], back_sem.at[1], {"sp": prv})

    def taps_rows(first, count):
        @pl.loop(first, first + count)
        def _(i):
            r0 = pl.multiple_of(i * 64, 64)

            @pl.loop(0, blocks)
            def _(cb):
                gc = gcpad[cb, pl.ds(r0, 64), :]
                for k in range(taps_n):
                    prod = gc * gpad[cb, pl.ds(r0 + HALO - taps_n + 1 + k, 64), :]
                    tacc[cb, k] += jnp.sum(prod.reshape(8, 8, LANES), axis=0)

    for k in range(zsize):
        pair_stage(k)
        if k == 1:
            send_back()
        if k >= 2:
            y_stage(k - 2)
    for j in range(1, chunks):
        gconv_chunk(j)
    y_stage(zsize - 2)

    steps = rows // 64
    taps_rows(0, steps // 2)
    z_stage(0)
    taps_rows(steps // 2, steps - steps // 2)

    small[...] = jnp.zeros_like(small)
    for cb in range(blocks):
        small[cb, pl.ds(0, taps_n + 2), :] = jnp.sum(tacc[cb], axis=1)
    to_pair = remote(
        small.at[pl.ds((1 - par) * half, half)], small_in, sp_sem.at[0], sp_sem.at[1],
        {"sp": partner},
    )
    to_pair.start()

    def gated_gradient(j):
        @pl.loop(0, LANES // 64)
        def _(h):
            r0 = pl.multiple_of(j * LANES + h * 64, 64)

            @pl.loop(0, blocks)
            def _(cb):
                acc = tap_row(0, cb) * gcpad[cb, pl.ds(r0 + taps_n - 1, 64), :]
                for k in range(1, taps_n):
                    acc = acc + tap_row(k, cb) * gcpad[cb, pl.ds(r0 + taps_n - 1 - k, 64), :]
                v = value[pl.ds(r0, 64), lanes(cb)].astype(F32)
                s = jax.nn.sigmoid(gate[pl.ds(r0, 64), lanes(cb)].astype(F32))
                ds = acc * s
                gv[pl.ds(r0, 64), lanes(cb)] = ds.astype(BF16)
                gg[pl.ds(r0, 64), lanes(cb)] = (ds * v * (1.0 - s)).astype(BF16)

    z_stage(1)
    to_pair.wait()
    small_y[cy] = small[pl.ds(par * half, half)] + small_in[...]

    def small_y_copy(i):
        return remote(
            small_y.at[cy], small_y.at[cy], sy_sem.at[0, i - 1], sy_sem.at[1, i - 1],
            {"sp": (cz * ysize + lax.rem(cy + i, ysize)) * 2 + par},
        )

    def small_z_copy(i):
        d = 2**i
        other = cz + d - 2 * d * lax.rem(cz // d, 2)
        return remote(
            small_z.at[i], small_zin.at[i], sz_sem.at[0, i], sz_sem.at[1, i],
            {"sp": (other * ysize + cy) * 2 + par},
        )

    for i in range(1, ysize):
        small_y_copy(i).start()
    y_stage(zsize - 1)

    gated_gradient(0)
    for k in range(2, zsize - 1):
        z_stage(k)
    gated_gradient(1)

    for i in range(1, ysize):
        small_y_copy(i).wait()
    total = small_y[0]
    for i in range(1, ysize):
        total = total + small_y[i]
    rounds = zsize.bit_length() - 1
    small_z[0] = total
    small_z_copy(0).start()

    for j in range(2, chunks - 1):
        gated_gradient(j)

    def next_round(i):
        small_z_copy(i).wait()
        both = small_z[i] + small_zin[i]
        if i + 1 < rounds:
            small_z[i + 1] = both
            small_z_copy(i + 1).start()
        return both

    back.wait()
    last = me == n - 1
    for cb in range(blocks):
        h = back_in[cb]
        gcpad[cb, pl.ds(rows, HALO), :] = jnp.where(last, jnp.zeros_like(h), h)
    gated_gradient(chunks - 1)

    z_stage(zsize - 1)
    for i in range(rounds):
        total = next_round(i)
    small_tot[...] = total
    fin = remote(small_tot, small_fin, sf_sem.at[0], sf_sem.at[1], {"sp": partner})
    fin.start()

    for k in range(zsize - 1):
        z_copy(k).wait()
        gp[...] += z_in[k].astype(F32)

    fin.wait()
    for cb in range(half):
        for source, where in ((small_tot, par), (small_fin, 1 - par)):
            cols = lanes(where * half + cb)
            taps_out[:, cols] = source[cb, pl.ds(0, taps_n), :]
            gain_out[:, cols] = source[cb, pl.ds(taps_n, 1), :]
            bias_out[:, cols] = source[cb, pl.ds(taps_n + 1, 1), :]


def write_out(*refs):
    sems = refs[12]
    copies = [pltpu.make_async_copy(refs[i], refs[6 + i], sems.at[i]) for i in range(6)]
    for c in copies:
        c.start()
    for c in copies:
        c.wait()


def on_device(n, tp, value, gate, taps, gain, bias, proj, grad):
    rows, width = value.shape
    model = grad.shape[1]
    taps_n = taps.shape[0]
    blocks = width // LANES
    chunks = rows // LANES
    nc = n // 2
    half = blocks // 2
    share = model // n
    ysize = 1
    while 2 * (2 * ysize) ** 2 <= nc:
        ysize *= 2
    zsize = nc // ysize
    hbm = pl.BlockSpec(memory_space=pltpu.HBM)
    vmem = pl.BlockSpec(memory_space=pltpu.VMEM)
    sem = pltpu.SemaphoreType.DMA
    wide = pltpu.VMEM((blocks, rows, LANES), F32)
    padded = pltpu.VMEM((blocks, rows + HALO, LANES), F32)
    gv, gg, gp, dtaps, dgain, dbias = pl.pallas_call(
        functools.partial(kernel, n, tp, taps_n, ysize),
        out_shape=(
            jax.ShapeDtypeStruct((rows, width), BF16),
            jax.ShapeDtypeStruct((rows, width), BF16),
            jax.ShapeDtypeStruct((share, width), F32),
            jax.ShapeDtypeStruct((taps_n, width), F32),
            jax.ShapeDtypeStruct((1, width), F32),
            jax.ShapeDtypeStruct((1, width), F32),
        ),
        in_specs=[hbm] * 7,
        out_specs=(vmem,) * 6,
        scratch_shapes=[
            pltpu.VMEM((rows, width), BF16),
            pltpu.VMEM((rows, width), BF16),
            pltpu.VMEM((taps_n, width), F32),
            pltpu.VMEM((1, width), F32),
            pltpu.VMEM((1, width), F32),
            pltpu.VMEM((width, model), BF16),
            pltpu.VMEM((rows, model), BF16),
            padded, wide, wide, wide, padded,
            pltpu.VMEM((rows, width), BF16),
            pltpu.VMEM((model, rows), BF16),
            pltpu.VMEM((n, share, width), F32),
            pltpu.VMEM((zsize, ysize, share, width), BF16),
            pltpu.VMEM((zsize, ysize, share, width), BF16),
            pltpu.VMEM((zsize, ysize - 1, share, width), BF16),
            pltpu.VMEM((zsize, ysize - 1, share, width), BF16),
            pltpu.VMEM((zsize - 1, share, width), BF16),
            pltpu.VMEM((zsize - 1, share, width), BF16),
            pltpu.VMEM((blocks, HALO, LANES), BF16),
            pltpu.VMEM((blocks, HALO, LANES), BF16),
            pltpu.VMEM((blocks, HALO, LANES), F32),
            pltpu.VMEM((blocks, HALO, LANES), F32),
            pltpu.VMEM((2, LANES, LANES), F32),
            pltpu.VMEM((LANES, LANES), F32),
            pltpu.VMEM((rows, LANES), F32),
            pltpu.VMEM((chunks, 8, LANES), F32),
            pltpu.VMEM((chunks, tp - 1, 8, LANES), F32),
            pltpu.VMEM((chunks, 8, LANES), F32),
            pltpu.VMEM((chunks, tp - 1, 8, LANES), F32),
            pltpu.VMEM((blocks, taps_n + 2, 8, LANES), F32),
            pltpu.VMEM((blocks, SMALL, LANES), F32),
            pltpu.VMEM((half, SMALL, LANES), F32),
            pltpu.VMEM((ysize, half, SMALL, LANES), F32),
            pltpu.VMEM((zsize.bit_length() - 1, half, SMALL, LANES), F32),
            pltpu.VMEM((zsize.bit_length() - 1, half, SMALL, LANES), F32),
            pltpu.VMEM((half, SMALL, LANES), F32),
            pltpu.VMEM((half, SMALL, LANES), F32),
            sem((7,)), sem((2,)), sem((2,)),
            sem((2, chunks, tp - 1)), sem((2, chunks, tp - 1)),
            sem((2, zsize)), sem((2, zsize, ysize - 1)), sem((2, zsize - 1)),
            sem((2,)), sem((2, ysize - 1)), sem((2, zsize.bit_length() - 1)), sem((2,)),
        ],
        compiler_params=pltpu.CompilerParams(
            collective_id=0, has_side_effects=True, vmem_limit_bytes=36 * 1024 * 1024
        ),
    )(
        *(
            pltpu.with_memory_space_constraint(x, pltpu.HBM)
            for x in (
                value, gate, taps, gain.reshape(1, width), bias.reshape(1, width), proj, grad
            )
        )
    )
    results = (gv, gg, gp, dtaps, dgain, dbias)
    gv, gg, gp, dtaps, dgain, dbias = pl.pallas_call(
        write_out,
        out_shape=[jax.ShapeDtypeStruct(r.shape, r.dtype) for r in results],
        in_specs=[pl.BlockSpec(memory_space=pl.ANY)] * 6,
        out_specs=[hbm] * 6,
        scratch_shapes=[sem((6,))],
        compiler_params=pltpu.CompilerParams(vmem_limit_bytes=1024 * 1024),
    )(*results)
    return gv, gg, dtaps, dgain.reshape(width), dbias.reshape(width), gp


def solution(mesh):
    n, tp = mesh.shape["sp"], mesh.shape["tp"]
    return jax.shard_map(
        functools.partial(on_device, n, tp),
        mesh=mesh,
        in_specs=(
            P("sp", "tp"),
            P("sp", "tp"),
            P(None, "tp"),
            P("tp"),
            P("tp"),
            P("tp", None),
            P("sp", None),
        ),
        out_specs=(P("sp", "tp"), P("sp", "tp"), P(None, "tp"), P("tp"), P("tp"), P("sp", "tp")),
        check_vma=False,
    )
```

```python
import functools

import jax
import jax.numpy as jnp
from jax import lax
from jax.experimental import pallas as pl
from jax.experimental.pallas import tpu as pltpu
from jax.sharding import PartitionSpec as P

LANES = 128
HALO = 32
SMALL = 40
MESH = pl.DeviceIdType.MESH
F32, BF16 = jnp.float32, jnp.bfloat16


def kernel(
    n, tp, taps_n, ysize,
    value_hbm, gate_hbm, taps_hbm, gain_hbm, bias_hbm, proj_hbm, grad_hbm,
    gv, gg, gp, taps_out, gain_out, bias_out,
    value, gate, taps_ref, gain_ref, bias_ref, proj, grad, gpad, conv, gact, gnorm, gcpad, act,
    grad_t, full, pair_out, pair_in, y_out, y_in, z_out, z_in,
    halo_out, halo_in, back_out, back_in,
    stage, mean_b, rstd_b, stat_out, stat_in, stat2_out, stat2_in,
    tacc, small, small_in, small_y, small_z, small_zin, small_fin, small_tot,
    in_sem, halo_sem, back_sem, stat_sem, stat2_sem,
    pair_sem, y_sem, z_sem, sp_sem, sy_sem, sz_sem, sf_sem,
):
    rows, width = value.shape
    blocks = width // LANES
    chunks = rows // LANES
    nc = n // 2
    half = blocks // 2
    share = full.shape[1]
    model = grad.shape[1]
    channels = width * tp
    me = lax.axis_index("sp")
    col = lax.axis_index("tp")
    par = lax.rem(me, 2)
    chip = me // 2
    partner = chip * 2 + 1 - par
    zsize = nc // ysize
    cy = lax.rem(chip, ysize)
    cz = chip // ysize
    zorder = list(range(zsize // 2, zsize)) + list(range(1, zsize // 2)) + [0]
    nxt = lax.rem(me + 1, n)
    prv = lax.rem(me + n - 1, n)

    loads = [
        pltpu.make_async_copy(s, d, in_sem.at[i])
        for i, (s, d) in enumerate(
            (
                (value_hbm, value), (gate_hbm, gate), (grad_hbm, grad), (proj_hbm, proj),
                (taps_hbm, taps_ref), (gain_hbm, gain_ref), (bias_hbm, bias_ref),
            )
        )
    ]
    for i in (0, 1, 4, 2, 3, 5, 6):
        loads[i].start()

    barrier = pltpu.get_barrier_semaphore()

    @pl.loop(1, n)
    def _(i):
        pl.semaphore_signal(
            barrier, inc=1, device_id={"sp": lax.rem(me + i, n)}, device_id_type=MESH
        )

    for t in range(1, tp):
        pl.semaphore_signal(
            barrier, inc=1, device_id={"tp": lax.rem(col + t, tp)}, device_id_type=MESH
        )

    def remote(src, dst, s, r, where):
        return pltpu.make_async_remote_copy(
            src_ref=src, dst_ref=dst, send_sem=s, recv_sem=r,
            device_id=where, device_id_type=MESH,
        )

    def lanes(cb):
        return pl.ds(pl.multiple_of(cb * LANES, LANES), LANES)

    def stat_copy(out, inn, sem, j, t):
        return remote(
            out.at[j], inn.at[j, t - 1], sem.at[0, j, t - 1], sem.at[1, j, t - 1],
            {"tp": lax.rem(col + t, tp)},
        )

    sub = lax.broadcasted_iota(jnp.int32, (8, LANES), 0)

    def send_stats(out, inn, sem, j):
        a = jnp.sum(stage[0].T, axis=0, keepdims=True)
        b = jnp.sum(stage[1].T, axis=0, keepdims=True)
        out[j] = jnp.where(sub == 0, a, b)
        for t in range(1, tp):
            stat_copy(out, inn, sem, j, t).start()

    def recv_stats(out, inn, sem, j):
        total = out[j]
        for t in range(1, tp):
            stat_copy(out, inn, sem, j, t).wait()
            total = total + inn[j, t - 1]
        total = total / channels
        return total[0:1], total[1:2]

    loads[0].wait()
    loads[1].wait()

    def gated_rows(r0, cb, count):
        v = value[pl.ds(r0, count), lanes(cb)].astype(F32)
        s = jax.nn.sigmoid(gate[pl.ds(r0, count), lanes(cb)].astype(F32))
        return (v * s).astype(BF16)

    for cb in range(blocks):
        g = gated_rows(rows - HALO, cb, HALO)
        halo_out[cb] = g
    halo = remote(halo_out, halo_in, halo_sem.at[0], halo_sem.at[1], {"sp": nxt})

    @pl.loop(0, rows // 64)
    def _(i):
        r0 = pl.multiple_of(i * 64, 64)
        for cb in range(blocks):
            gpad[cb, pl.ds(r0 + HALO, 64), :] = gated_rows(r0, cb, 64).astype(F32)

    def tap_row(k, cb):
        return taps_ref[pl.ds(k, 1), lanes(cb)]

    def conv_chunk(j):
        for h in range(LANES // 64):
            r0 = j * LANES + h * 64

            def body(cb, carry):
                s, q = carry
                step = (j * (LANES // 64) + h) * blocks + cb
                tiles = []
                for e in range(per_step):
                    tile = step * per_step + e
                    across = pl.ds(pl.multiple_of(tile % chunks * LANES, LANES), LANES)
                    down = pl.ds(pl.multiple_of(tile // chunks * LANES, LANES), LANES)
                    tiles.append((down, across, grad[across, down].T))
                acc = tap_row(0, cb) * gpad[cb, pl.ds(r0 + 2, 64), :]
                for k in range(1, taps_n):
                    acc = acc + tap_row(k, cb) * gpad[cb, pl.ds(r0 + HALO - taps_n + 1 + k, 64), :]
                conv[cb, pl.ds(r0, 64), :] = acc
                for down, across, tile in tiles:
                    grad_t[down, across] = tile
                return s + acc, q + acc * acc

            zero = jnp.zeros((64, LANES), F32)
            s, q = lax.fori_loop(0, blocks, body, (zero, zero))
            stage[0, pl.ds(h * 64, 64), :] = s
            stage[1, pl.ds(h * 64, 64), :] = q
        if j == 1:
            pl.semaphore_wait(barrier, n - 1 + tp - 1)
            halo.start()
        send_stats(stat_out, stat_in, stat_sem, j)

    order = list(range(1, chunks)) + [0]
    per_step = (model // LANES) * chunks // (chunks * (LANES // 64) * blocks)
    loads[4].wait()
    loads[2].wait()
    for j in order:
        if j == 0:
            halo.wait()
            first = me == 0
            for cb in range(blocks):
                h = halo_in[cb].astype(F32)
                gpad[cb, pl.ds(0, HALO), :] = jnp.where(first, jnp.zeros_like(h), h)
        conv_chunk(j)

    loads[3].wait()
    loads[5].wait()
    loads[6].wait()
    for cb in range(0, blocks, 2):
        both = lax.dot_general(
            grad[...], proj[pl.ds(cb * LANES, 2 * LANES), :], (((1,), (1,)), ((), ())),
            preferred_element_type=F32,
        )
        gact[cb] = both[:, :LANES]
        gact[cb + 1] = both[:, LANES:]

    tacc[...] = jnp.zeros_like(tacc)

    def norm_chunk(j):
        mean, sq = recv_stats(stat_out, stat_in, stat_sem, j)
        rstd = lax.rsqrt(sq - mean * mean + 1e-05)
        mean_b[...] = jnp.broadcast_to(mean, (LANES, LANES)).T
        rstd_b[pl.ds(j * LANES, LANES), :] = jnp.broadcast_to(rstd, (LANES, LANES)).T

        @pl.loop(0, LANES // 32)
        def _(h):
            l0 = pl.multiple_of(h * 32, 32)
            r0 = pl.multiple_of(j * LANES + l0, 32)
            m = mean_b[pl.ds(l0, 32), :]
            rs = rstd_b[pl.ds(r0, 32), :]
            s1 = jnp.zeros((32, LANES), F32)
            s2 = jnp.zeros((32, LANES), F32)
            for cb in range(blocks):
                cols = pl.ds(cb * LANES, LANES)
                gain = gain_ref[:, cols]
                xhat = (conv[cb, pl.ds(r0, 32), :] - m) * rs
                nrm = xhat * gain + bias_ref[:, cols]
                sig = jax.nn.sigmoid(nrm)
                act[pl.ds(r0, 32), cols] = (nrm * sig).astype(BF16)
                gn = gact[cb, pl.ds(r0, 32), :] * sig * (1.0 + nrm * (1.0 - sig))
                conv[cb, pl.ds(r0, 32), :] = xhat
                gx = gn * gain
                gnorm[cb, pl.ds(r0, 32), :] = gx
                gxx = gx * xhat
                s1 = s1 + gx
                s2 = s2 + gxx
                tacc[cb, taps_n] += jnp.sum((gn * xhat).reshape(4, 8, LANES), axis=0)
                tacc[cb, taps_n + 1] += jnp.sum(gn.reshape(4, 8, LANES), axis=0)
            stage[0, pl.ds(l0, 32), :] = s1
            stage[1, pl.ds(l0, 32), :] = s2

        send_stats(stat2_out, stat2_in, stat2_sem, j)

    for j in order:
        norm_chunk(j)

    def owners(k):
        return lax.rem(cz + zorder[k], zsize) * 2 * ysize

    def pair_copy(k):
        return remote(
            pair_out.at[k], pair_in.at[k], pair_sem.at[0, k], pair_sem.at[1, k],
            {"sp": partner},
        )

    def y_copy(k, i):
        return remote(
            y_out.at[k, i - 1], y_in.at[k, i - 1], y_sem.at[0, k, i - 1],
            y_sem.at[1, k, i - 1],
            {"sp": (cz * ysize + lax.rem(cy + i, ysize)) * 2 + par},
        )

    def z_copy(k):
        return remote(
            z_out.at[k], z_in.at[k], z_sem.at[0, k], z_sem.at[1, k],
            {"sp": (lax.rem(cz + zorder[k], zsize) * ysize + cy) * 2 + par},
        )

    def pair_stage(k):
        base = owners(k)
        span = 2 * ysize * share
        part = lax.dot_general(
            grad_t[pl.ds(pl.multiple_of(base * share, LANES), span), :], act[...],
            (((1,), (0,)), ((), ())), preferred_element_type=F32,
        )
        full[pl.ds(base, 2 * ysize)] = part.reshape(2 * ysize, share, width)
        for y in range(ysize):
            pair_out[k, y] = full[base + 2 * y + 1 - par].astype(BF16)
        pair_copy(k).start()

    def y_stage(k):
        base = owners(k)
        pair_copy(k).wait()
        for i in range(1, ysize):
            y = lax.rem(cy + i, ysize)
            y_out[k, i - 1] = (full[base + 2 * y + par] + pair_in[k, y].astype(F32)).astype(BF16)
            y_copy(k, i).start()

    def z_stage(k):
        acc = full[owners(k) + 2 * cy + par] + pair_in[k, cy].astype(F32)
        for i in range(1, ysize):
            y_copy(k, i).wait()
            acc = acc + y_in[k, i - 1].astype(F32)
        if zorder[k]:
            z_out[k] = acc.astype(BF16)
            z_copy(k).start()
        else:
            gp[...] = acc

    def gconv_chunk(j):
        m1, m2 = recv_stats(stat2_out, stat2_in, stat2_sem, j)
        stage[0] = jnp.broadcast_to(m1, (LANES, LANES)).T
        stage[1] = jnp.broadcast_to(m2, (LANES, LANES)).T

        @pl.loop(0, LANES // 64)
        def _(h):
            l0 = pl.multiple_of(h * 64, 64)
            r0 = pl.multiple_of(j * LANES + l0, 64)
            a = stage[0, pl.ds(l0, 64), :]
            b = stage[1, pl.ds(l0, 64), :]
            rs = rstd_b[pl.ds(r0, 64), :]
            for cb in range(blocks):
                gcpad[cb, pl.ds(r0, 64), :] = rs * (
                    gnorm[cb, pl.ds(r0, 64), :] - a - conv[cb, pl.ds(r0, 64), :] * b
                )

    def send_back():
        gconv_chunk(0)
        for cb in range(blocks):
            back_out[cb] = gcpad[cb, pl.ds(0, HALO), :]
        back.start()

    back = remote(back_out, back_in, back_sem.at[0], back_sem.at[1], {"sp": prv})

    def taps_rows(first, count):
        @pl.loop(first, first + count)
        def _(i):
            r0 = pl.multiple_of(i * 64, 64)

            @pl.loop(0, blocks)
            def _(cb):
                gc = gcpad[cb, pl.ds(r0, 64), :]
                for k in range(taps_n):
                    prod = gc * gpad[cb, pl.ds(r0 + HALO - taps_n + 1 + k, 64), :]
                    tacc[cb, k] += jnp.sum(prod.reshape(8, 8, LANES), axis=0)

    for k in range(zsize):
        pair_stage(k)
        if k == 1:
            send_back()
        if k >= 2:
            y_stage(k - 2)
    for j in range(1, chunks):
        gconv_chunk(j)
    y_stage(zsize - 2)

    steps = rows // 64
    taps_rows(0, steps)

    small[...] = jnp.zeros_like(small)
    for cb in range(blocks):
        small[cb, pl.ds(0, taps_n + 2), :] = jnp.sum(tacc[cb], axis=1)
    to_pair = remote(
        small.at[pl.ds((1 - par) * half, half)], small_in, sp_sem.at[0], sp_sem.at[1],
        {"sp": partner},
    )
    to_pair.start()

    def gated_gradient(j):
        @pl.loop(0, LANES // 64)
        def _(h):
            r0 = pl.multiple_of(j * LANES + h * 64, 64)

            @pl.loop(0, blocks)
            def _(cb):
                acc = tap_row(0, cb) * gcpad[cb, pl.ds(r0 + taps_n - 1, 64), :]
                for k in range(1, taps_n):
                    acc = acc + tap_row(k, cb) * gcpad[cb, pl.ds(r0 + taps_n - 1 - k, 64), :]
                v = value[pl.ds(r0, 64), lanes(cb)].astype(F32)
                s = jax.nn.sigmoid(gate[pl.ds(r0, 64), lanes(cb)].astype(F32))
                ds = acc * s
                gv[pl.ds(r0, 64), lanes(cb)] = ds.astype(BF16)
                gg[pl.ds(r0, 64), lanes(cb)] = (ds * v * (1.0 - s)).astype(BF16)

    z_stage(0)
    gated_gradient(0)
    z_stage(1)
    to_pair.wait()
    small_y[cy] = small[pl.ds(par * half, half)] + small_in[...]

    def small_y_copy(i):
        return remote(
            small_y.at[cy], small_y.at[cy], sy_sem.at[0, i - 1], sy_sem.at[1, i - 1],
            {"sp": (cz * ysize + lax.rem(cy + i, ysize)) * 2 + par},
        )

    def small_z_copy(i):
        d = 2**i
        other = cz + d - 2 * d * lax.rem(cz // d, 2)
        return remote(
            small_z.at[i], small_zin.at[i], sz_sem.at[0, i], sz_sem.at[1, i],
            {"sp": (other * ysize + cy) * 2 + par},
        )

    for i in range(1, ysize):
        small_y_copy(i).start()
    y_stage(zsize - 1)

    for k in range(2, zsize - 1):
        z_stage(k)
    gated_gradient(1)

    for i in range(1, ysize):
        small_y_copy(i).wait()
    total = small_y[0]
    for i in range(1, ysize):
        total = total + small_y[i]
    rounds = zsize.bit_length() - 1
    small_z[0] = total
    small_z_copy(0).start()

    for j in range(2, chunks - 1):
        gated_gradient(j)

    def next_round(i):
        small_z_copy(i).wait()
        both = small_z[i] + small_zin[i]
        if i + 1 < rounds:
            small_z[i + 1] = both
            small_z_copy(i + 1).start()
        return both

    back.wait()
    last = me == n - 1
    for cb in range(blocks):
        h = back_in[cb]
        gcpad[cb, pl.ds(rows, HALO), :] = jnp.where(last, jnp.zeros_like(h), h)
    gated_gradient(chunks - 1)

    z_stage(zsize - 1)
    for i in range(rounds):
        total = next_round(i)
    small_tot[...] = total
    fin = remote(small_tot, small_fin, sf_sem.at[0], sf_sem.at[1], {"sp": partner})
    fin.start()

    for k in range(zsize - 1):
        z_copy(k).wait()
        gp[...] += z_in[k].astype(F32)

    fin.wait()
    for cb in range(half):
        for source, where in ((small_tot, par), (small_fin, 1 - par)):
            cols = lanes(where * half + cb)
            taps_out[:, cols] = source[cb, pl.ds(0, taps_n), :]
            gain_out[:, cols] = source[cb, pl.ds(taps_n, 1), :]
            bias_out[:, cols] = source[cb, pl.ds(taps_n + 1, 1), :]


def write_out(*refs):
    sems = refs[12]
    copies = [pltpu.make_async_copy(refs[i], refs[6 + i], sems.at[i]) for i in range(6)]
    for c in copies:
        c.start()
    for c in copies:
        c.wait()


def on_device(n, tp, value, gate, taps, gain, bias, proj, grad):
    rows, width = value.shape
    model = grad.shape[1]
    taps_n = taps.shape[0]
    blocks = width // LANES
    chunks = rows // LANES
    nc = n // 2
    half = blocks // 2
    share = model // n
    ysize = 1
    while 2 * (2 * ysize) ** 2 <= nc:
        ysize *= 2
    zsize = nc // ysize
    hbm = pl.BlockSpec(memory_space=pltpu.HBM)
    vmem = pl.BlockSpec(memory_space=pltpu.VMEM)
    sem = pltpu.SemaphoreType.DMA
    wide = pltpu.VMEM((blocks, rows, LANES), F32)
    padded = pltpu.VMEM((blocks, rows + HALO, LANES), F32)
    gv, gg, gp, dtaps, dgain, dbias = pl.pallas_call(
        functools.partial(kernel, n, tp, taps_n, ysize),
        out_shape=(
            jax.ShapeDtypeStruct((rows, width), BF16),
            jax.ShapeDtypeStruct((rows, width), BF16),
            jax.ShapeDtypeStruct((share, width), F32),
            jax.ShapeDtypeStruct((taps_n, width), F32),
            jax.ShapeDtypeStruct((1, width), F32),
            jax.ShapeDtypeStruct((1, width), F32),
        ),
        in_specs=[hbm] * 7,
        out_specs=(vmem,) * 6,
        scratch_shapes=[
            pltpu.VMEM((rows, width), BF16),
            pltpu.VMEM((rows, width), BF16),
            pltpu.VMEM((taps_n, width), F32),
            pltpu.VMEM((1, width), F32),
            pltpu.VMEM((1, width), F32),
            pltpu.VMEM((width, model), BF16),
            pltpu.VMEM((rows, model), BF16),
            padded, wide, wide, wide, padded,
            pltpu.VMEM((rows, width), BF16),
            pltpu.VMEM((model, rows), BF16),
            pltpu.VMEM((n, share, width), F32),
            pltpu.VMEM((zsize, ysize, share, width), BF16),
            pltpu.VMEM((zsize, ysize, share, width), BF16),
            pltpu.VMEM((zsize, ysize - 1, share, width), BF16),
            pltpu.VMEM((zsize, ysize - 1, share, width), BF16),
            pltpu.VMEM((zsize - 1, share, width), BF16),
            pltpu.VMEM((zsize - 1, share, width), BF16),
            pltpu.VMEM((blocks, HALO, LANES), BF16),
            pltpu.VMEM((blocks, HALO, LANES), BF16),
            pltpu.VMEM((blocks, HALO, LANES), F32),
            pltpu.VMEM((blocks, HALO, LANES), F32),
            pltpu.VMEM((2, LANES, LANES), F32),
            pltpu.VMEM((LANES, LANES), F32),
            pltpu.VMEM((rows, LANES), F32),
            pltpu.VMEM((chunks, 8, LANES), F32),
            pltpu.VMEM((chunks, tp - 1, 8, LANES), F32),
            pltpu.VMEM((chunks, 8, LANES), F32),
            pltpu.VMEM((chunks, tp - 1, 8, LANES), F32),
            pltpu.VMEM((blocks, taps_n + 2, 8, LANES), F32),
            pltpu.VMEM((blocks, SMALL, LANES), F32),
            pltpu.VMEM((half, SMALL, LANES), F32),
            pltpu.VMEM((ysize, half, SMALL, LANES), F32),
            pltpu.VMEM((zsize.bit_length() - 1, half, SMALL, LANES), F32),
            pltpu.VMEM((zsize.bit_length() - 1, half, SMALL, LANES), F32),
            pltpu.VMEM((half, SMALL, LANES), F32),
            pltpu.VMEM((half, SMALL, LANES), F32),
            sem((7,)), sem((2,)), sem((2,)),
            sem((2, chunks, tp - 1)), sem((2, chunks, tp - 1)),
            sem((2, zsize)), sem((2, zsize, ysize - 1)), sem((2, zsize - 1)),
            sem((2,)), sem((2, ysize - 1)), sem((2, zsize.bit_length() - 1)), sem((2,)),
        ],
        compiler_params=pltpu.CompilerParams(
            collective_id=0, has_side_effects=True, vmem_limit_bytes=36 * 1024 * 1024
        ),
    )(
        *(
            pltpu.with_memory_space_constraint(x, pltpu.HBM)
            for x in (
                value, gate, taps, gain.reshape(1, width), bias.reshape(1, width), proj, grad
            )
        )
    )
    results = (gv, gg, gp, dtaps, dgain, dbias)
    gv, gg, gp, dtaps, dgain, dbias = pl.pallas_call(
        write_out,
        out_shape=[jax.ShapeDtypeStruct(r.shape, r.dtype) for r in results],
        in_specs=[pl.BlockSpec(memory_space=pl.ANY)] * 6,
        out_specs=[hbm] * 6,
        scratch_shapes=[sem((6,))],
        compiler_params=pltpu.CompilerParams(vmem_limit_bytes=1024 * 1024),
    )(*results)
    return gv, gg, dtaps, dgain.reshape(width), dbias.reshape(width), gp


def solution(mesh):
    n, tp = mesh.shape["sp"], mesh.shape["tp"]
    return jax.shard_map(
        functools.partial(on_device, n, tp),
        mesh=mesh,
        in_specs=(
            P("sp", "tp"),
            P("sp", "tp"),
            P(None, "tp"),
            P("tp"),
            P("tp"),
            P("tp", None),
            P("sp", None),
        ),
        out_specs=(P("sp", "tp"), P("sp", "tp"), P(None, "tp"), P("tp"), P("tp"), P("sp", "tp")),
        check_vma=False,
    )
```
